32 devices in a mesh: sp: 4 (over z), fs: 4 (over y, core), tp: 2 (over x).
Axes of the slice: x: 2, y: 2, z: 4, core: 2. Of those that a mesh axis runs over, the one named last changes fastest.
Arguments:
- tokens: bfloat16 [4, 4096, 2048], P('fs', 'sp', 'tp'), may hold values from -8 to 8
- norm_gain: float32 [2048], replicated, may hold values from 0.1 to 1.9
- w_query: bfloat16 [2048, 1024], P(('sp', 'fs'), 'tp'), may hold values from -4 to 4
- w_key: bfloat16 [2048, 512], P(('sp', 'fs'), 'tp'), may hold values from -0.16 to 0.16
- w_value: bfloat16 [2048, 512], P(('sp', 'fs'), 'tp'), may hold values from -0.125 to 0.125
- w_conv_in: bfloat16 [2048, 1024], P(('sp', 'fs'), 'tp'), may hold values from -0.125 to 0.125
- w_conv_b: bfloat16 [2048, 1024], P(('sp', 'fs'), 'tp'), may hold values from -0.125 to 0.125
- w_conv_c: bfloat16 [2048, 1024], P(('sp', 'fs'), 'tp'), may hold values from -0.125 to 0.125
- conv_taps: bfloat16 [3, 1024], P(None, 'tp'), may hold values from -3.5 to 3.5
- sink_logits: float32 [16], P('tp'), may hold values from 1 to 5
- w_attn_out: bfloat16 [1024, 2048], P('tp', ('sp', 'fs')), may hold values from -0.375 to 0.375
- w_conv_out: bfloat16 [1024, 2048], P('tp', ('sp', 'fs')), may hold values from -0.125 to 0.125
Outputs:
- mixed: bfloat16 [4, 4096, 2048], P('fs', ('sp', 'tp'))
The draws below stay inside these ranges and needn't reach their ends.
All inputs are finite; a program needn't handle non-finite values.
Results may differ from the reference program's by a relative error of at most 0.02.
Values may be sent and summed in bfloat16 or wider, within the bound.
No kernel may reach another device: no remote copies, remote signals or barrier semaphores. Data moves between devices by JAX's collectives and lax.ppermute only.
A program may use at most 128 MiB of HBM per device.

```python
import jax
import jax.numpy as jnp
from jax import lax

D = 2048
HEADS = 16
KV_HEADS = 8
HEAD = 64
CONV = 1024
WINDOW = 128
SEQS = 4
LENGTH = 4096
N_TP = 2


def query_key_pair(key):
    folded = jax.random.fold_in(key, 11)
    first, second = jax.random.split(folded, 2)
    key_weights = jnp.clip(jax.random.normal(first, (D, KV_HEADS * HEAD), jnp.float32) * D ** (-0.5), -0.15, 0.15)
    query_weights = jax.random.normal(second, (D, HEADS * HEAD), jnp.float32) * D ** (-0.5)
    query_weights = jnp.clip(query_weights, -4.0, 4.0)
    return (query_weights, key_weights)


def draw_w_query(key, part):
    return query_key_pair(key)[0].astype(jnp.bfloat16)


def draw_w_key(key, part):
    return query_key_pair(key)[1].astype(jnp.bfloat16)


def draw_tokens(key, part):
    folded = jax.random.fold_in(key, 23)
    first = jax.random.fold_in(folded, 0)
    values = jax.random.normal(first, (SEQS, LENGTH, D), jnp.float32)
    return jnp.clip(values, -8.0, 8.0).astype(jnp.bfloat16)


def block_levels(own_key, extent, shards, least, top_value):
    def one(axis_at, shards_of):
        heights = jax.random.uniform(jax.random.fold_in(jax.random.fold_in(own_key, 6), axis_at), (shards_of,), jnp.float32, least / len(shards), top_value / len(shards))
        return jnp.repeat(jnp.exp(heights), extent[axis_at] // shards_of).reshape((-1,) + (1,) * (len(extent) - axis_at - 1))

    gain = one(*shards[0])
    for cut in shards[1:]:
        gain = gain * one(*cut)
    return gain


def normal_values(key, dims, deviation, bound, shards=(), kind=jnp.bfloat16):
    entries = jax.random.normal(key, dims, jnp.float32) * deviation
    if len(shards) > 0:
        entries = block_levels(key, dims, shards, -0.22, 0.18) * entries
    return jnp.clip(entries, min=-bound, max=bound).astype(kind)


def setup_inputs(seed: int = 0) -> dict:
    key_list = jax.random.split(jax.random.key(seed), 13)
    return {
        "tokens": draw_tokens(jax.random.fold_in(key_list[12], 71), 0),
        "norm_gain": jnp.clip(1.0 + 0.18 * jax.random.normal(key_list[1], (D,), jnp.float32), 0.1, 1.9),
        "w_query": draw_w_query(jax.random.fold_in(key_list[12], 71), 0),
        "w_key": draw_w_key(jax.random.fold_in(key_list[12], 71), 0),
        "w_value": normal_values(key_list[4], (D, KV_HEADS * HEAD), D ** -0.5, 0.125, ((0, 16), (1, 2))),
        "w_conv_in": normal_values(key_list[5], (D, CONV), D ** -0.5, 0.125, ((0, 16), (1, 2))),
        "w_conv_b": normal_values(key_list[6], (D, CONV), D ** -0.5, 0.125, ((0, 16), (1, 2))),
        "w_conv_c": normal_values(key_list[7], (D, CONV), D ** -0.5, 0.125, ((0, 16), (1, 2))),
        "conv_taps": normal_values(key_list[8], (3, CONV), 3 ** -0.5, 3.5, ((1, 2),)),
        "sink_logits": jnp.clip(1.0 + 4.0 * jax.random.uniform(key_list[9], (HEADS,), jnp.float32) ** block_levels(key_list[9], (HEADS,), ((0, 2),), -0.2, 0.2), 1.0, 5.0),
        "w_attn_out": normal_values(key_list[10], (HEADS * HEAD, D), (D // 8) ** -0.5, 0.375, ((0, 2), (1, 16))),
        "w_conv_out": normal_values(key_list[11], (CONV, D), D ** -0.5, 0.125, ((0, 2), (1, 16))),
    }


def norm_rows(tokens, norm_gain):
    values = tokens.astype(jnp.float32)
    average = lax.optimization_barrier(jnp.mean(values, axis=-1, keepdims=True))
    centred = values - average
    variance = lax.optimization_barrier(jnp.mean(centred * centred, axis=-1, keepdims=True))
    return (centred * lax.rsqrt(variance + 1e-05) * norm_gain.astype(jnp.float32)).astype(jnp.bfloat16)

def project(normed, weight):
    return jnp.dot(normed, weight, preferred_element_type=jnp.float32).astype(jnp.bfloat16)

def window_attention(queries, keys, values, sink_logits):
    length = queries.shape[0]
    blocks = length // WINDOW
    group = HEADS // KV_HEADS
    query_form = queries.astype(jnp.float32).reshape(blocks, WINDOW, KV_HEADS, group, HEAD)
    zero_rows = jnp.zeros((WINDOW, KV_HEADS * HEAD), jnp.bfloat16)
    padded_keys = jnp.concatenate([zero_rows, keys], axis=0).astype(jnp.float32).reshape(blocks + 1, WINDOW, KV_HEADS, HEAD)
    padded_values = jnp.concatenate([zero_rows, values], axis=0).astype(jnp.float32).reshape(blocks + 1, WINDOW, KV_HEADS, HEAD)
    band_keys = jnp.concatenate([padded_keys[:-1], padded_keys[1:]], axis=1)
    band_values = jnp.concatenate([padded_values[:-1], padded_values[1:]], axis=1)
    scores = jnp.einsum('bqkgd,bskd->bkgqs', query_form, band_keys) * HEAD ** (-0.5)
    row_ids = jnp.arange(WINDOW, dtype=jnp.int32)[:, None]
    col_ids = jnp.arange(2 * WINDOW, dtype=jnp.int32)[None, :]
    distance = WINDOW + row_ids - col_ids
    head_ids = jnp.arange(HEADS, dtype=jnp.int32).reshape(KV_HEADS, group)
    slopes = jnp.exp2(-8.0 * (head_ids + 1).astype(jnp.float32) / HEADS)
    scores = scores - slopes[:, :, None, None] * distance.astype(jnp.float32)
    key_place = jnp.arange(blocks, dtype=jnp.int32)[:, None] * WINDOW - WINDOW + jnp.arange(2 * WINDOW, dtype=jnp.int32)[None, :]
    inside = (distance >= 0) & (distance < WINDOW)
    keep = inside[None, None, None, :, :] & (key_place >= 0)[:, None, None, None, :]
    scores = jnp.where(keep, scores, -jnp.inf)
    sinks = sink_logits.astype(jnp.float32).reshape(KV_HEADS, group)[:, :, None, None]
    highest = jnp.maximum(lax.optimization_barrier(jnp.max(scores, axis=-1, keepdims=True)), sinks)
    raised = jnp.exp(scores - highest)
    denominator = lax.optimization_barrier(jnp.sum(raised, axis=-1, keepdims=True)) + jnp.exp(sinks - highest)
    weights = (raised / denominator).astype(jnp.bfloat16)
    mixed = jnp.einsum('bkgqs,bskd->bqkgd', weights.astype(jnp.float32), band_values)
    return mixed.astype(jnp.bfloat16).reshape(length, HEADS * HEAD)

def reference(tokens, norm_gain, w_query, w_key, w_value, w_conv_in, w_conv_b, w_conv_c, conv_taps, sink_logits, w_attn_out, w_conv_out):
    normed_all = norm_rows(tokens, norm_gain)
    head_cols = HEADS * HEAD // N_TP
    chan_cols = CONV // N_TP
    taps = conv_taps.astype(jnp.float32)

    def one_sequence(normed):
        queries = project(normed, w_query)
        keys = project(normed, w_key)
        values = project(normed, w_value)
        inner = project(normed, w_conv_in)
        gate_b = project(normed, w_conv_b)
        gate_c = project(normed, w_conv_c)
        attended = window_attention(queries, keys, values, sink_logits)
        product = (gate_c.astype(jnp.float32) * inner.astype(jnp.float32)).astype(jnp.bfloat16)
        padded = jnp.concatenate([jnp.zeros((2, CONV), jnp.float32), product.astype(jnp.float32)], axis=0)
        length = product.shape[0]
        filtered = taps[0] * padded[0:length] + taps[1] * padded[1:length + 1] + taps[2] * padded[2:length + 2]
        conv_out = (gate_b.astype(jnp.float32) * filtered).astype(jnp.bfloat16)
        summed = jnp.zeros((length, D), jnp.float32)
        for group_id in range(N_TP):
            head_slice = slice(group_id * head_cols, (group_id + 1) * head_cols)
            chan_slice = slice(group_id * chan_cols, (group_id + 1) * chan_cols)
            partial_sum = jnp.dot(attended[:, head_slice], w_attn_out[head_slice], preferred_element_type=jnp.float32)
            partial_sum = partial_sum + jnp.dot(conv_out[:, chan_slice], w_conv_out[chan_slice], preferred_element_type=jnp.float32)
            summed = summed + partial_sum.astype(jnp.bfloat16).astype(jnp.float32)
        return summed.astype(jnp.bfloat16)
    return lax.map(one_sequence, normed_all)
```

```python
import jax
import jax.numpy as jnp
from jax import lax
from jax.sharding import PartitionSpec as P

HEADS = 16
HEAD = 64
WINDOW = 128


def shifted(block, axis, distance):
    devices = range(lax.axis_size(axis))
    route = [(i - distance, i) for i in devices if i - distance in devices]
    return lax.ppermute(block, axis, route)


def norm_rows(tokens, norm_gain):
    values = tokens.astype(jnp.float32)
    average = jnp.mean(values, axis=-1, keepdims=True)
    centred = values - average
    variance = jnp.mean(centred * centred, axis=-1, keepdims=True)
    return (centred * lax.rsqrt(variance + 1e-05) * norm_gain).astype(jnp.bfloat16)


def attend_block(queries, band, sink_logits, head_base, row_base):
    block_rows = queries.shape[0]
    kv_cols = band.shape[1] // 2
    kv_here = kv_cols // HEAD
    heads_here = queries.shape[1] // HEAD
    group = heads_here // kv_here
    head_ids = head_base + jnp.arange(heads_here, dtype=jnp.int32)
    slopes = jnp.exp2(-8.0 * (head_ids + 1).astype(jnp.float32) / HEADS).reshape(kv_here, group)[
        :, :, None, None
    ]
    sinks = sink_logits.reshape(kv_here, group)[:, :, None, None]
    row_ids = jnp.arange(block_rows, dtype=jnp.int32)[:, None]
    col_ids = jnp.arange(block_rows + WINDOW, dtype=jnp.int32)[None, :]
    distance = WINDOW + row_ids - col_ids
    query_block = queries.reshape(block_rows, kv_here, group, HEAD)
    band_keys = band[:, :kv_cols].reshape(block_rows + WINDOW, kv_here, HEAD)
    band_values = band[:, kv_cols:].reshape(block_rows + WINDOW, kv_here, HEAD)
    scores = jnp.einsum(
        "qkgd,skd->kgqs", query_block, band_keys, preferred_element_type=jnp.float32
    ) * HEAD ** (-0.5)
    scores = scores - slopes * distance.astype(jnp.float32)
    key_place = row_base - WINDOW + col_ids
    keep = (distance >= 0) & (distance < WINDOW) & (key_place >= 0)
    scores = jnp.where(keep, scores, -jnp.inf)
    highest = jnp.maximum(jnp.max(scores, axis=-1, keepdims=True), sinks)
    raised = jnp.exp(scores - highest)
    denominator = jnp.sum(raised, axis=-1, keepdims=True) + jnp.exp(sinks - highest)
    weights = (raised / denominator).astype(jnp.bfloat16)
    mixed = jnp.einsum("kgqs,skd->qkgd", weights, band_values, preferred_element_type=jnp.float32)
    return mixed.astype(jnp.bfloat16).reshape(block_rows, heads_here * HEAD)


def gather_features(block, axis):
    size = lax.axis_size(axis)
    here = lax.axis_index(axis)
    cols = block.shape[1]
    whole = jnp.zeros((block.shape[0], cols * size), block.dtype)
    whole = lax.dynamic_update_slice(whole, block, (0, here * cols))
    for step in range(1, size):
        other = lax.ppermute(block, axis, [(i, (i + step) % size) for i in range(size)])
        whole = lax.dynamic_update_slice(whole, other, (0, (here - step) % size * cols))
    return whole


def gather_weights(in_part, out_parts):
    in_rows = lax.all_gather(in_part, ("sp", "fs"), axis=0, tiled=True)
    out_part = jnp.concatenate(out_parts, axis=0)
    return in_rows, lax.all_gather(out_part, ("sp", "fs"), axis=1, tiled=True)


def on_device(
    tokens,
    norm_gain,
    w_query,
    w_key,
    w_value,
    w_conv_in,
    w_conv_b,
    w_conv_c,
    conv_taps,
    sink_logits,
    w_attn_out,
    w_conv_out,
):
    ins = (w_key, w_value, w_conv_in, w_conv_c, w_query, w_conv_b)
    in_rows, out_columns = gather_weights(jnp.concatenate(ins, axis=1), (w_attn_out, w_conv_out))
    normed = norm_rows(gather_features(tokens[0], "tp"), norm_gain)
    row_total = normed.shape[0]
    projected = jnp.dot(normed, in_rows, preferred_element_type=jnp.float32).astype(jnp.bfloat16)
    stops = [0]
    for part in ins:
        stops.append(stops[-1] + part.shape[1])
    _, _, inner, gate_c, queries, gate_b = (projected[:, i:j] for i, j in zip(stops, stops[1:]))
    keys_values = projected[:, : stops[2]]
    product = (gate_c.astype(jnp.float32) * inner.astype(jnp.float32)).astype(jnp.bfloat16)
    earlier_kv, earlier_product = shifted(
        (keys_values[row_total - WINDOW :], product[row_total - 2 :]), "sp", 1
    )
    kv_all = jnp.concatenate([earlier_kv, keys_values], axis=0)
    padded = jnp.concatenate([earlier_product, product], axis=0)
    size = lax.axis_size("tp")
    here = lax.axis_index("tp")
    heads_here = queries.shape[1] // HEAD
    row_base = lax.axis_index("sp") * row_total
    taps = conv_taps.astype(jnp.float32)
    rows = row_total // size

    def partial(first):
        attended = attend_block(
            lax.dynamic_slice_in_dim(queries, first, rows, 0),
            lax.dynamic_slice_in_dim(kv_all, first, rows + WINDOW, 0),
            sink_logits,
            here * heads_here,
            row_base + first,
        )
        near = lax.dynamic_slice_in_dim(padded, first, rows + 2, 0).astype(jnp.float32)
        filtered = taps[0] * near[:rows] + taps[1] * near[1 : rows + 1] + taps[2] * near[2:]
        gate = lax.dynamic_slice_in_dim(gate_b, first, rows, 0).astype(jnp.float32)
        conv_out = (gate * filtered).astype(jnp.bfloat16)
        both = jnp.concatenate([attended, conv_out], axis=1)
        return jnp.dot(both, out_columns, preferred_element_type=jnp.float32).astype(jnp.bfloat16)

    arrived = []
    for step in range(1, size):
        piece = partial((here + step) % size * rows)
        piece, queries, kv_all, padded, gate_b = lax.optimization_barrier(
            (piece, queries, kv_all, padded, gate_b)
        )
        arrived.append(lax.ppermute(piece, "tp", [(i, (i + step) % size) for i in range(size)]))
    summed = partial(here * rows).astype(jnp.float32)
    for piece in arrived:
        summed = summed + piece.astype(jnp.float32)
    return summed.astype(jnp.bfloat16)[None]


def solution(mesh):
    placed = (
        P("fs", "sp", "tp"),
        P(),
        P(("sp", "fs"), "tp"),
        P(("sp", "fs"), "tp"),
        P(("sp", "fs"), "tp"),
        P(("sp", "fs"), "tp"),
        P(("sp", "fs"), "tp"),
        P(("sp", "fs"), "tp"),
        P(None, "tp"),
        P("tp"),
        P("tp", ("sp", "fs")),
        P("tp", ("sp", "fs")),
    )
    return jax.shard_map(
        on_device,
        mesh=mesh,
        in_specs=placed,
        out_specs=P("fs", ("sp", "tp"), None),
        check_vma=False,
    )
```
